32 devices in a mesh: ep: 8 (over z, y), tp: 4 (over x, core).
Axes of the slice: x: 2, y: 2, z: 4, core: 2. Of those that a mesh axis runs over, the one named last changes fastest.
Arguments:
- tokens: bfloat16 [128, 4096], P('ep'), may hold values from -6 to 6
- norm_gain: float32 [4096], replicated, may hold values from 0.1 to 1.9
- token_expert_index: int32 [128, 4], P('ep'), may hold values from 0 to 7, as said below
- group_prob: float32 [128], P('ep'), may hold values from 0.25 to 1
- expert_weight: float32 [128, 4], P('ep'), may hold values from 0.05 to 1
- w_gate: bfloat16 [8, 4096, 2048], P('ep', None, 'tp'), may hold values from -0.09375 to 0.09375
- w_up: bfloat16 [8, 4096, 2048], P('ep', None, 'tp'), may hold values from -0.09375 to 0.09375
- w_down: bfloat16 [8, 2048, 4096], P('ep', 'tp'), may hold values from -0.125 to 0.125
Outputs:
- mixed: bfloat16 [128, 4096], P('ep', 'tp')
The draws below stay inside these ranges and needn't reach their ends.
Inputs may be any that keep to these rules, and one draw needn't show every extreme that they name: `token_expert_index`: each row names 4 different experts, all of one group: the group g holds experts g * 4 to (g + 1) * 4 - 1. The 16 rows of one index of ep name any one expert at most 16 times.
All inputs are finite; a program needn't handle non-finite values.
Results may differ from the reference program's by a relative error of at most 0.019.
Values may be sent and summed in bfloat16 or wider, within the bound.
A program may use at most 64 MiB of HBM per device.

```python
import math
import jax
import jax.numpy as jnp
from jax import lax

D = 4096
FF = 2048
TOK_DEV = 16
TOPK = 4
GROUPS = 2
EXPERTS = 8
CAP = 16
TOKENS = 128
N_EP = 8
N_TP = 4


def draw_token_expert_index(key, part):
    blocks = TOKENS // TOK_DEV
    per_group = EXPERTS // GROUPS
    keys = jax.random.split(jax.random.fold_in(key, 11), 4)
    hottest = jax.random.randint(keys[0], (), 0, EXPERTS)
    favored_experts = jax.random.randint(keys[1], (EXPERTS,), 0, 4)
    extra_reward = jnp.where(favored_experts == 0, 3000, 0).astype(jnp.int32)
    group_draw = jax.random.randint(keys[2], (TOK_DEV, blocks), 0, GROUPS)
    noise = jax.random.randint(keys[3], (TOK_DEV, blocks, per_group), 0, 2000)
    block_ids = jnp.arange(blocks, dtype=jnp.int32)
    position = jnp.arange(TOK_DEV, dtype=jnp.int32)[:, None]
    after = jnp.broadcast_to((block_ids + 1) % EXPERTS, (TOK_DEV, blocks))
    across = jnp.broadcast_to((block_ids + EXPERTS // 2) % EXPERTS, (TOK_DEV, blocks))
    target = jnp.where(position == 0, after, jnp.where(position == 1, across, jnp.where((position >= 2) & (position < 2 + CAP), hottest, -1)))
    groups = jnp.where(target >= 0, target // per_group, group_draw)
    local = jnp.arange(per_group, dtype=jnp.int32)
    everyone = jnp.arange(EXPERTS, dtype=jnp.int32)

    def one_token(counts, inputs):
        grp, destination_index, coarse_estimate = inputs
        candidate_experts = grp[:, None] * per_group + local[None, :]
        used = jnp.take_along_axis(counts, candidate_experts, axis=1)
        baseline_score = coarse_estimate + extra_reward[candidate_experts] + jnp.where(candidate_experts == destination_index[:, None], 100000, 0)
        baseline_score = jnp.where(used >= CAP, -1, baseline_score)
        score = baseline_score * per_group + local[None, :]
        _, picked = lax.top_k(score, TOPK)
        chosen = (grp[:, None] * per_group + picked).astype(jnp.int32)
        counts = counts + jnp.sum((chosen[:, :, None] == everyone[None, None, :]).astype(jnp.int32), axis=1)
        return (counts, chosen)
    start = jnp.zeros((blocks, EXPERTS), jnp.int32)
    _, result = lax.scan(one_token, start, (groups, target, noise))
    return jnp.transpose(result, (1, 0, 2)).reshape(TOKENS, TOPK).astype(jnp.int32)


def levels(rng, shape, cuts, smallest, largest):
    def one(dim, blocks):
        draws = jax.random.uniform(jax.random.fold_in(jax.random.fold_in(rng, 6), dim), (blocks,), jnp.float32, smallest / len(cuts), largest / len(cuts))
        return jnp.repeat(jnp.exp(draws), shape[dim] // blocks).reshape((-1,) + (1,) * (len(shape) - dim - 1))

    level = one(*cuts[0])
    for cut in cuts[1:]:
        level = level * one(*cut)
    return level


def centred(stream_key, shape, scale, bound, cuts=(), kind=jnp.bfloat16):
    level = levels(stream_key, shape, cuts, -0.22, 0.18) if cuts else 1.0
    drawn = jax.random.normal(stream_key, shape, jnp.float32) * scale * level
    return jnp.minimum(jnp.maximum(drawn, -bound), bound).astype(kind)


def setup_inputs(seed: int = 0) -> dict:
    key_list = jax.random.split(jax.random.key(seed), 9)
    tokens = centred(key_list[0], (TOKENS, D), 1.0, 6.0, ((0, 8),))
    norm_gain = jnp.clip(1.0 + 0.18 * jax.random.normal(key_list[1], (D,), jnp.float32), 0.1, 1.9)
    token_expert_index = draw_token_expert_index(jax.random.fold_in(key_list[8], 71), 0)
    group_prob = jnp.clip(0.25 + 0.75 * jax.random.uniform(key_list[3], (TOKENS,), jnp.float32) ** levels(key_list[3], (TOKENS,), ((0, 8),), -0.2, 0.2), 0.25, 1.0)
    expert_weight = jnp.clip(jnp.exp(math.log(1.0) - 2.9957323 * jax.random.uniform(key_list[4], (TOKENS, TOPK), jnp.float32) ** levels(key_list[4], (TOKENS, TOPK), ((0, 8),), -0.2, 0.2)), 0.05, 1.0)
    w_gate = centred(key_list[5], (EXPERTS, D, FF), D ** -0.5, 0.09375, ((0, 8), (2, 4)))
    w_up = centred(key_list[6], (EXPERTS, D, FF), D ** -0.5, 0.09375, ((0, 8), (2, 4)))
    w_down = centred(key_list[7], (EXPERTS, FF, D), FF ** -0.5, 0.125, ((0, 8), (1, 4)))
    return {"tokens": tokens, "norm_gain": norm_gain, "token_expert_index": token_expert_index, "group_prob": group_prob, "expert_weight": expert_weight, "w_gate": w_gate, "w_up": w_up, "w_down": w_down}


def reference(tokens, norm_gain, token_expert_index, group_prob, expert_weight, w_gate, w_up, w_down):
    xf = tokens.astype(jnp.float32)
    normed = (xf * lax.rsqrt(lax.optimization_barrier(jnp.mean(xf * xf, axis=-1, keepdims=True)) + 1e-06) * norm_gain).astype(jnp.bfloat16)
    gates = group_prob[:, None] * expert_weight / lax.optimization_barrier(jnp.sum(expert_weight, axis=-1, keepdims=True))
    limit = N_EP * CAP
    padded = jnp.concatenate([normed, jnp.zeros((1, D), jnp.bfloat16)], axis=0)

    def one_expert(carry, inputs):
        gate_mat, up_mat, down_mat, number = inputs
        hits = token_expert_index == number
        weight = lax.optimization_barrier(jnp.sum(jnp.where(hits, gates, jnp.float32(0.0)), axis=1))
        weight = jnp.concatenate([weight, jnp.zeros((1,), jnp.float32)])
        rows = jnp.nonzero(jnp.any(hits, axis=1), size=limit, fill_value=TOKENS)[0].astype(jnp.int32)
        chosen = padded[rows]
        gate = jnp.dot(chosen, gate_mat, preferred_element_type=jnp.float32)
        upper = jnp.dot(chosen, up_mat, preferred_element_type=jnp.float32)
        hidden = (jax.nn.silu(gate) * upper).astype(jnp.bfloat16)
        blocks = hidden.reshape(limit, N_TP, FF // N_TP).astype(jnp.float32)
        downs = down_mat.reshape(N_TP, FF // N_TP, D).astype(jnp.float32)
        parts = jnp.einsum('rnf,nfd->nrd', blocks, downs).astype(jnp.bfloat16)
        parts = lax.optimization_barrier(parts).astype(jnp.float32)
        output = lax.optimization_barrier(jnp.sum(parts, axis=0)).astype(jnp.bfloat16).astype(jnp.float32)
        carry = carry.at[rows].add(output * weight[rows][:, None])
        return (carry, None)
    start = jnp.zeros((TOKENS + 1, D), jnp.float32)
    numbers = jnp.arange(EXPERTS, dtype=jnp.int32)
    total, _ = lax.scan(one_expert, start, (w_gate, w_up, w_down, numbers))
    return total[:TOKENS].astype(jnp.bfloat16)
```

```python
import functools

import jax
import jax.numpy as jnp
from jax import lax
from jax.experimental import pallas as pl
from jax.experimental.pallas import tpu as pltpu
from jax.sharding import PartitionSpec as P

GROUPS = 2


def general(tokens, norm_gain, token_expert_index, group_prob, expert_weight, w_gate, w_up, w_down):
    rows_here, width = tokens.shape
    topk = token_expert_index.shape[1]
    experts = lax.axis_size("ep")
    tp_count = lax.axis_size("tp")
    per_group = experts // GROUPS
    capacity = min(rows_here, max(2, rows_here * topk // max(per_group - topk, 1) + 1))
    xf = tokens.astype(jnp.float32)
    normed = (xf * lax.rsqrt(jnp.mean(xf * xf, axis=-1, keepdims=True) + 1e-06) * norm_gain).astype(
        jnp.bfloat16
    )
    gates = group_prob[:, None] * expert_weight / jnp.sum(expert_weight, axis=-1, keepdims=True)
    flattened_index = token_expert_index.reshape(-1)
    onehot = (flattened_index[:, None] == jnp.arange(experts, dtype=jnp.int32)[None, :]).astype(
        jnp.int32
    )
    earlier = jnp.cumsum(onehot, axis=0) - onehot
    slot_rank = jnp.sum(earlier * onehot, axis=1)
    place = flattened_index * capacity + slot_rank
    slots_total = experts * capacity
    select = (jnp.arange(slots_total, dtype=jnp.int32)[:, None] == place[None, :]).astype(
        jnp.float32
    )
    select = jnp.sum(select.reshape(slots_total, rows_here, topk), axis=2).astype(jnp.bfloat16)
    outgoing = jnp.dot(select, normed, preferred_element_type=jnp.float32).astype(jnp.bfloat16)
    share = width // tp_count
    arrived = lax.all_to_all(outgoing, "ep", split_axis=0, concat_axis=0, tiled=True)
    gate = jnp.dot(arrived, w_gate[0], preferred_element_type=jnp.float32)
    upper = jnp.dot(arrived, w_up[0], preferred_element_type=jnp.float32)
    hidden = (jax.nn.silu(gate) * upper).astype(jnp.bfloat16)
    partial_out = jnp.dot(hidden, w_down[0], preferred_element_type=jnp.float32)
    mine = lax.psum_scatter(partial_out.astype(jnp.bfloat16), "tp", scatter_dimension=1, tiled=True)
    returned = lax.all_to_all(mine, "ep", split_axis=0, concat_axis=0, tiled=True)
    picked = returned[place].astype(jnp.float32).reshape(rows_here, topk, share)
    mixed = jnp.sum(picked * gates[:, :, None], axis=1)
    return mixed.astype(jnp.bfloat16)


MESH = pl.DeviceIdType.MESH
CHUNKS = 4
LANES = 128


def kernel(dims, tokens, gain, index, group_prob, weight, wg_hbm, wu_hbm, wd_hbm, out, xg, wg, wu, wd,
           table, acc_g, acc_u, hid, csend, crecv, ckeep, xsend, xrecv, xkeep, ysend, yrecv, zsend, zrecv, zkeep,
           wsem, gz, gy, gx, gc, gd, tz, ty, sc, sx, sy, sz):
    nz, ny, rows, share, chunk = dims
    ep, t = lax.axis_index("ep"), lax.axis_index("tp")
    z, y = ep // ny, ep % ny
    x, c = t // 2, t % 2
    yo = 1 - y
    t_core, t_x, t_diag = x * 2 + (1 - c), (1 - x) * 2 + c, (1 - x) * 2 + (1 - c)
    half = nz * rows
    y_dev = {"ep": z * ny + yo, "tp": t}
    x_dev = {"ep": ep, "tp": t_x}
    core_dev = {"ep": ep, "tp": t_core}

    def z_dev(d):
        return {"ep": ((z + d) % nz) * ny + y, "tp": t}

    loads = [
        pltpu.make_async_copy(wg_hbm.at[0], wg, wsem.at[0]),
        pltpu.make_async_copy(wu_hbm.at[0], wu, wsem.at[1]),
        pltpu.make_async_copy(wd_hbm.at[0], wd, wsem.at[2]),
    ]
    for load in loads:
        load.start()

    barrier = pltpu.get_barrier_semaphore()
    peers = [z_dev(d) for d in range(1, nz)] + [y_dev, x_dev, core_dev]
    for peer in peers:
        pl.semaphore_signal(barrier, inc=1, device_id=peer, device_id_type=MESH)

    def place(zz, yy):
        return pl.ds(pl.multiple_of((yy * nz + zz) * rows, rows), rows)

    xf = tokens[...].astype(jnp.float32)
    scale = lax.rsqrt(jnp.mean(xf * xf, axis=-1, keepdims=True) + 1e-06)
    normed = (xf * scale * gain[...]).astype(jnp.bfloat16)
    for q in range(xg.shape[0]):
        xg[q, place(z, y), :] = normed[:, q * share : (q + 1) * share]
    ew = weight[...]
    gates = group_prob[...] * ew / jnp.sum(ew, axis=-1, keepdims=True)
    lane = lax.broadcasted_iota(jnp.int32, (rows, LANES), 1)
    own = jnp.zeros((rows, LANES), jnp.float32)
    for k in range(ew.shape[1]):
        own = own + jnp.where(index[:, k : k + 1] == lane, gates[:, k : k + 1], 0.0)
    table[place(z, y), :] = own
    pl.semaphore_wait(barrier, len(peers))

    sent = []

    def send(src, dst, sems, i, device):
        copy = pltpu.make_async_remote_copy(
            src_ref=src, dst_ref=dst, send_sem=sems.at[0, i], recv_sem=sems.at[1, i],
            device_id=device, device_id_type=MESH,
        )
        copy.start()
        sent.append(copy)

    def arrive(dst, sems, i):
        pltpu.make_async_remote_copy(
            src_ref=dst, dst_ref=dst, send_sem=sems.at[0, i], recv_sem=sems.at[1, i],
            device_id=y_dev, device_id_type=MESH,
        ).wait_recv()

    def block(q, zz, yy):
        return xg.at[q, place(zz, yy)]

    def from_z(d):
        return (z + nz - d) % nz

    mine = block(t, z, y)
    for d in range(1, nz):
        send(mine, mine, gz, d, z_dev(d))
    send(mine, mine, gy, 0, y_dev)
    my_table = table.at[place(z, y)]
    for d in range(1, nz):
        send(my_table, my_table, tz, d, z_dev(d))
    send(my_table, my_table, ty, 0, y_dev)

    def spread(got, i):
        send(got, got, gx, i, x_dev)
        send(got, got, gc, i, core_dev)

    got = block(t, z, yo)
    arrive(got, gy, 0)
    spread(got, nz)
    for d in range(1, nz):
        got = block(t, from_z(d), y)
        arrive(got, gz, d)
        send(got, got, gy, d, y_dev)
        spread(got, d)
    for d in range(1, nz):
        got = block(t, from_z(d), yo)
        arrive(got, gy, d)
        spread(got, nz + d)
    for d in range(1, nz):
        got = table.at[place(from_z(d), y)]
        arrive(got, tz, d)
        send(got, got, ty, d, y_dev)

    def which(i):
        return (from_z(i % nz), y if i < nz else yo)

    order = [nz] + list(range(1, nz)) + list(range(nz + 1, 2 * nz))

    def project(q, first):
        lhs = xg[q]
        span = pl.ds(pl.multiple_of(q * share, share), share)
        for acc, w in ((acc_g, wg), (acc_u, wu)):
            value = jnp.dot(lhs, w[span, :], preferred_element_type=jnp.float32)
            acc[...] = value if first else acc[...] + value

    loads[0].wait()
    loads[1].wait()
    project(t, True)
    for i in order:
        got = block(t_x, *which(i))
        arrive(got, gx, i)
        send(got, got, gd, i, core_dev)
    for i in order:
        arrive(block(t_core, *which(i)), gc, i)
    project(t_core, False)
    project(t_x, False)
    for d in range(nz):
        arrive(table.at[place(from_z(d), yo)], ty, d)
    for i in order:
        arrive(block(t_diag, *which(i)), gd, i)
    project(t_diag, False)

    lanes = lax.broadcasted_iota(jnp.int32, table.shape, 1)
    factor = jnp.sum(jnp.where(lanes == ep, table[...], 0.0), axis=1, keepdims=True)
    gate = acc_g[...]
    hid[...] = (gate / (1.0 + jnp.exp(-gate)) * acc_u[...] * factor).astype(jnp.bfloat16)

    loads[2].wait()

    def down(xq, cq, j):
        start = pl.multiple_of((xq * 2 + cq) * share + j * chunk, chunk)
        return jnp.dot(hid[...], wd[:, pl.ds(start, chunk)], preferred_element_type=jnp.float32)

    for j in range(CHUNKS):
        csend[0, j] = down(1 - x, 1 - c, j).astype(jnp.bfloat16)
        send(csend.at[0, j], crecv.at[0, j], sc, j, core_dev)
    for j in range(CHUNKS):
        ckeep[0, j] = down(1 - x, c, j)
    for j in range(CHUNKS):
        arrive(crecv.at[0, j], sc, j)
        xsend[j] = (ckeep[0, j] + crecv[0, j].astype(jnp.float32)).astype(jnp.bfloat16)
        send(xsend.at[j], xrecv.at[j], sx, j, x_dev)
    for j in range(CHUNKS):
        csend[1, j] = down(x, 1 - c, j).astype(jnp.bfloat16)
        send(csend.at[1, j], crecv.at[1, j], sc, CHUNKS + j, core_dev)
    for j in range(CHUNKS):
        ckeep[1, j] = down(x, c, j)
    for j in range(CHUNKS):
        arrive(crecv.at[1, j], sc, CHUNKS + j)
        ckeep[1, j] = ckeep[1, j] + crecv[1, j].astype(jnp.float32)

    ours, theirs = pl.ds(pl.multiple_of(y * half, half), half), pl.ds(pl.multiple_of(yo * half, half), half)

    def after_x(j):
        arrive(xrecv.at[j], sx, j)
        ysend[j] = (ckeep[1, j, theirs, :] + xrecv[j, theirs, :].astype(jnp.float32)).astype(jnp.bfloat16)
        send(ysend.at[j], yrecv.at[j], sy, j, y_dev)
        xkeep[j] = ckeep[1, j, ours, :] + xrecv[j, ours, :].astype(jnp.float32)

    def after_y(j):
        arrive(yrecv.at[j], sy, j)
        total = xkeep[j] + yrecv[j].astype(jnp.float32)
        zkeep[j] = total
        zsend[j] = total.astype(jnp.bfloat16)
        for d in range(1, nz):
            src = zsend.at[j, pl.ds(pl.multiple_of(((z + d) % nz) * rows, rows), rows)]
            send(src, zrecv.at[j, d - 1], sz, j * nz + d, z_dev(d))

    for j in range(CHUNKS):
        after_x(j)
        if j:
            after_y(j - 1)
    after_y(CHUNKS - 1)
    for j in range(CHUNKS):
        total = zkeep[j, pl.ds(pl.multiple_of(z * rows, rows), rows), :]
        for d in range(1, nz):
            arrive(zrecv.at[j, d - 1], sz, j * nz + d)
            total = total + zrecv[j, d - 1].astype(jnp.float32)
        out[:, j * chunk : (j + 1) * chunk] = total.astype(jnp.bfloat16)
    for copy in sent:
        copy.wait_send()


def fused(tokens, norm_gain, token_expert_index, group_prob, expert_weight, w_gate, w_up, w_down):
    rows, width = tokens.shape
    n_ep, n_tp = lax.axis_size("ep"), lax.axis_size("tp")
    ny = 2
    nz = n_ep // ny
    share, hidden = width // n_tp, w_gate.shape[2]
    chunk = share // CHUNKS
    all_rows = n_ep * rows
    half = nz * rows
    bf, f32 = jnp.bfloat16, jnp.float32
    vmem, dma = pltpu.VMEM, pltpu.SemaphoreType.DMA
    return pl.pallas_call(
        functools.partial(kernel, (nz, ny, rows, share, chunk)),
        out_shape=jax.ShapeDtypeStruct((rows, share), bf),
        in_specs=[pl.BlockSpec(memory_space=vmem)] * 5 + [pl.BlockSpec(memory_space=pl.ANY)] * 3,
        out_specs=pl.BlockSpec(memory_space=vmem),
        scratch_shapes=[
            vmem((n_tp, all_rows, share), bf),
            vmem(w_gate.shape[1:], bf), vmem(w_up.shape[1:], bf), vmem(w_down.shape[1:], bf),
            vmem((all_rows, LANES), f32),
            vmem((all_rows, hidden), f32), vmem((all_rows, hidden), f32), vmem((all_rows, hidden), bf),
            vmem((2, CHUNKS, all_rows, chunk), bf), vmem((2, CHUNKS, all_rows, chunk), bf),
            vmem((2, CHUNKS, all_rows, chunk), f32),
            vmem((CHUNKS, all_rows, chunk), bf), vmem((CHUNKS, all_rows, chunk), bf),
            vmem((CHUNKS, half, chunk), f32),
            vmem((CHUNKS, half, chunk), bf), vmem((CHUNKS, half, chunk), bf),
            vmem((CHUNKS, half, chunk), bf), vmem((CHUNKS, nz - 1, rows, chunk), bf),
            vmem((CHUNKS, half, chunk), f32),
            dma((3,)), dma((2, nz)), dma((2, nz)), dma((2, 2 * nz)), dma((2, 2 * nz)), dma((2, 2 * nz)),
            dma((2, nz)), dma((2, nz)),
            dma((2, 2 * CHUNKS)), dma((2, CHUNKS)), dma((2, CHUNKS)), dma((2, CHUNKS * nz)),
        ],
        compiler_params=pltpu.CompilerParams(
            collective_id=0, has_side_effects=True, vmem_limit_bytes=48 * 1024 * 1024
        ),
    )(tokens, norm_gain[None, :], token_expert_index, group_prob[:, None], expert_weight, w_gate, w_up, w_down)


def slots(rows, topk, experts):
    return min(rows, max(2, rows * topk // max(experts // GROUPS - topk, 1) + 1))


def body(*args):
    tokens, topk = args[0], args[2].shape[1]
    n_ep, n_tp = lax.axis_size("ep"), lax.axis_size("tp")
    rows, width = tokens.shape
    dense = slots(rows, topk, n_ep) == rows and n_ep % 2 == 0 and n_ep <= LANES and n_tp == 4
    if dense and rows % 16 == 0 and width % (n_tp * CHUNKS * LANES) == 0:
        return fused(*args)
    return general(*args)


def solution(mesh):
    return jax.shard_map(
        body,
        mesh=mesh,
        in_specs=(
            P("ep", None),
            P(),
            P("ep", None),
            P("ep"),
            P("ep", None),
            P("ep", None, "tp"),
            P("ep", None, "tp"),
            P("ep", "tp", None),
        ),
        out_specs=P("ep", "tp"),
        check_vma=False,
    )
```

```python
import functools

import jax
import jax.numpy as jnp
from jax import lax
from jax.experimental import pallas as pl
from jax.experimental.pallas import tpu as pltpu
from jax.sharding import PartitionSpec as P

GROUPS = 2


def general(tokens, norm_gain, token_expert_index, group_prob, expert_weight, w_gate, w_up, w_down):
    rows_here, width = tokens.shape
    topk = token_expert_index.shape[1]
    experts = lax.axis_size("ep")
    tp_count = lax.axis_size("tp")
    per_group = experts // GROUPS
    capacity = min(rows_here, max(2, rows_here * topk // max(per_group - topk, 1) + 1))
    xf = tokens.astype(jnp.float32)
    normed = (xf * lax.rsqrt(jnp.mean(xf * xf, axis=-1, keepdims=True) + 1e-06) * norm_gain).astype(
        jnp.bfloat16
    )
    gates = group_prob[:, None] * expert_weight / jnp.sum(expert_weight, axis=-1, keepdims=True)
    flattened_index = token_expert_index.reshape(-1)
    onehot = (flattened_index[:, None] == jnp.arange(experts, dtype=jnp.int32)[None, :]).astype(
        jnp.int32
    )
    earlier = jnp.cumsum(onehot, axis=0) - onehot
    slot_rank = jnp.sum(earlier * onehot, axis=1)
    place = flattened_index * capacity + slot_rank
    slots_total = experts * capacity
    select = (jnp.arange(slots_total, dtype=jnp.int32)[:, None] == place[None, :]).astype(
        jnp.float32
    )
    select = jnp.sum(select.reshape(slots_total, rows_here, topk), axis=2).astype(jnp.bfloat16)
    outgoing = jnp.dot(select, normed, preferred_element_type=jnp.float32).astype(jnp.bfloat16)
    share = width // tp_count
    arrived = lax.all_to_all(outgoing, "ep", split_axis=0, concat_axis=0, tiled=True)
    gate = jnp.dot(arrived, w_gate[0], preferred_element_type=jnp.float32)
    upper = jnp.dot(arrived, w_up[0], preferred_element_type=jnp.float32)
    hidden = (jax.nn.silu(gate) * upper).astype(jnp.bfloat16)
    partial_out = jnp.dot(hidden, w_down[0], preferred_element_type=jnp.float32)
    mine = lax.psum_scatter(partial_out.astype(jnp.bfloat16), "tp", scatter_dimension=1, tiled=True)
    returned = lax.all_to_all(mine, "ep", split_axis=0, concat_axis=0, tiled=True)
    picked = returned[place].astype(jnp.float32).reshape(rows_here, topk, share)
    mixed = jnp.sum(picked * gates[:, :, None], axis=1)
    return mixed.astype(jnp.bfloat16)


MESH = pl.DeviceIdType.MESH
CHUNKS = 2
LANES = 128


def kernel(dims, tokens_hbm, gain_hbm, index_hbm, prob_hbm, weight_hbm, wg_hbm, wu_hbm, wd_hbm, out,
           tokens, gain, index, group_prob, weight, xg, wg, wu, wd, table, acc_g, acc_u, hid, csend, crecv, ckeep, bsend, ysend, brecv, zsend, zrecv, zkeep,
           wsem, gz, gy, gx, gw, gc, gd, tz, ty, sc, sb, sz):
    nz, ny, rows, share, chunk = dims
    ep, t = lax.axis_index("ep"), lax.axis_index("tp")
    z, y = ep // ny, ep % ny
    x, c = t // 2, t % 2
    yo = 1 - y
    t_core, t_x, t_diag = x * 2 + (1 - c), (1 - x) * 2 + c, (1 - x) * 2 + (1 - c)
    half = nz * rows
    y_dev = {"ep": z * ny + yo, "tp": t}
    x_dev = {"ep": ep, "tp": t_x}
    core_dev = {"ep": ep, "tp": t_core}

    diag_dev = {"ep": z * ny + yo, "tp": t_x}

    def flip(d):
        return sum(
            (1 << b) * (1 - (z // (1 << b)) % 2 if d >> b & 1 else (z // (1 << b)) % 2) for b in range(nz.bit_length() - 1)
        )

    def z_dev(d):
        return {"ep": flip(d) * ny + y, "tp": t}

    loads = [
        pltpu.make_async_copy(wg_hbm.at[0], wg, wsem.at[0]),
        pltpu.make_async_copy(wu_hbm.at[0], wu, wsem.at[1]),
        pltpu.make_async_copy(wd_hbm.at[0], wd, wsem.at[2]),
    ]
    small = [
        pltpu.make_async_copy(src, dst, wsem.at[3 + i])
        for i, (src, dst) in enumerate(
            ((tokens_hbm, tokens), (gain_hbm, gain), (index_hbm, index), (prob_hbm, group_prob), (weight_hbm, weight))
        )
    ]
    for load in small + loads:
        load.start()

    barrier = pltpu.get_barrier_semaphore()
    peers = [z_dev(d) for d in range(1, nz)] + [y_dev, x_dev, diag_dev, core_dev]
    for peer in peers:
        pl.semaphore_signal(barrier, inc=1, device_id=peer, device_id_type=MESH)

    def place(zz, yy):
        return pl.ds(pl.multiple_of((yy * nz + zz) * rows, rows), rows)

    for load in small:
        load.wait()
    xf = tokens[...].astype(jnp.float32)
    scale = lax.rsqrt(jnp.mean(xf * xf, axis=-1, keepdims=True) + 1e-06)
    normed = (xf * scale * gain[...]).astype(jnp.bfloat16)
    for q in range(xg.shape[0]):
        xg[q, place(z, y), :] = normed[:, q * share : (q + 1) * share]
    ew = weight[...]
    gates = group_prob[...] * ew / jnp.sum(ew, axis=0, keepdims=True)
    expert = lax.broadcasted_iota(jnp.int32, (table.shape[1], rows), 0)
    own = jnp.zeros(expert.shape, jnp.float32)
    for k in range(ew.shape[0]):
        own = own + jnp.where(index[k : k + 1, :] == expert, gates[k : k + 1, :], 0.0)
    table[y * nz + z] = jnp.zeros(table.shape[1:], jnp.float32)
    table[y * nz + z, :, :rows] = own
    pl.semaphore_wait(barrier, len(peers))

    sent = []

    def send(src, dst, sems, i, device):
        copy = pltpu.make_async_remote_copy(
            src_ref=src, dst_ref=dst, send_sem=sems.at[0, i], recv_sem=sems.at[1, i],
            device_id=device, device_id_type=MESH,
        )
        copy.start()
        sent.append(copy)

    def arrive(dst, sems, i):
        pltpu.make_async_remote_copy(
            src_ref=dst, dst_ref=dst, send_sem=sems.at[0, i], recv_sem=sems.at[1, i],
            device_id=y_dev, device_id_type=MESH,
        ).wait_recv()

    def block(q, zz, yy):
        return xg.at[q, place(zz, yy)]

    mine = block(t, z, y)
    for d in range(nz - 1, 0, -1):
        send(mine, mine, gz, d, z_dev(d))
    send(mine, mine, gy, 0, y_dev)
    other = block(t_x, z, y)
    send(other, other, gy, nz, y_dev)
    my_table = table.at[y * nz + z]
    for d in range(1, nz):
        send(my_table, my_table, tz, d, z_dev(d))
    send(my_table, my_table, ty, 0, y_dev)

    def relay(got, sems, i, onward, k):
        arrive(got, sems, i)
        send(got, got, onward, k, core_dev)

    relay(block(t, z, yo), gy, 0, gc, nz)
    relay(block(t_x, z, yo), gy, nz, gd, nz)
    for d in range(1, nz):
        got = block(t, flip(d), y)
        arrive(got, gz, d)
        send(got, got, gw, d, diag_dev)
        send(got, got, gy, d, y_dev)
        send(got, got, gx, d, x_dev)
        send(got, got, gc, d, core_dev)
    for d in range(1, nz):
        got = table.at[y * nz + flip(d)]
        arrive(got, tz, d)
        send(got, got, ty, d, y_dev)

    def which(i):
        return (flip(i % nz), y if i < nz else yo)

    order = [nz] + list(range(1, nz)) + list(range(nz + 1, 2 * nz))

    def project(q, first):
        lhs = xg[q]
        span = pl.ds(pl.multiple_of(q * share, share), share)
        for acc, w in ((acc_g, wg), (acc_u, wu)):
            value = jnp.dot(lhs, w[span, :], preferred_element_type=jnp.float32)
            acc[...] = value if first else acc[...] + value

    loads[0].wait()
    loads[1].wait()
    for d in range(1, nz):
        relay(block(t_x, flip(d), y), gx, d, gd, d)
        relay(block(t, flip(d), yo), gy, d, gc, nz + d)
    project(t, True)
    for d in range(1, nz):
        relay(block(t_x, flip(d), yo), gw, d, gd, nz + d)
    for i in order:
        arrive(block(t_core, *which(i)), gc, i)
    project(t_core, False)
    project(t_x, False)
    for d in range(nz):
        arrive(table.at[yo * nz + flip(d)], ty, d)
    for i in order:
        arrive(block(t_diag, *which(i)), gd, i)
    project(t_diag, False)

    diagonal = lax.broadcasted_iota(jnp.int32, (rows, rows), 0) == lax.broadcasted_iota(jnp.int32, (rows, rows), 1)
    factor = jnp.concatenate(
        [
            jnp.sum(jnp.where(diagonal, table[b, pl.ds(ep, 1), :rows], 0.0), axis=1, keepdims=True)
            for b in range(table.shape[0])
        ],
        axis=0,
    )
    gate = acc_g[...]
    hid[...] = (gate / (1.0 + jnp.exp(-gate)) * acc_u[...] * factor).astype(jnp.bfloat16)

    loads[2].wait()

    def down(xq, cq, j):
        start = pl.multiple_of((xq * 2 + cq) * share + j * chunk, chunk)
        return jnp.dot(hid[...], wd[:, pl.ds(start, chunk)], preferred_element_type=jnp.float32)

    ours, theirs = pl.ds(pl.multiple_of(y * half, half), half), pl.ds(pl.multiple_of(yo * half, half), half)
    for j in range(CHUNKS):
        csend[0, j] = down(1 - x, 1 - c, j).astype(jnp.bfloat16)
        send(csend.at[0, j], crecv.at[0, j], sc, j, core_dev)
    for j in range(CHUNKS):
        ckeep[0, j] = down(1 - x, c, j)
    for j in range(CHUNKS):
        arrive(crecv.at[0, j], sc, j)
        bsend[j] = (ckeep[0, j] + crecv[0, j].astype(jnp.float32)).astype(jnp.bfloat16)
        send(bsend.at[j, theirs], brecv.at[1, j], sb, CHUNKS + j, diag_dev)
        send(bsend.at[j, ours], brecv.at[0, j], sb, j, x_dev)
    for j in range(CHUNKS):
        csend[1, j] = down(x, 1 - c, j).astype(jnp.bfloat16)
        send(csend.at[1, j], crecv.at[1, j], sc, CHUNKS + j, core_dev)
    for j in range(CHUNKS):
        ckeep[1, j] = down(x, c, j)
    for j in range(CHUNKS):
        arrive(crecv.at[1, j], sc, CHUNKS + j)
        ysend[j] = (ckeep[1, j, theirs, :] + crecv[1, j, theirs, :].astype(jnp.float32)).astype(jnp.bfloat16)
        send(ysend.at[j], brecv.at[2, j], sb, 2 * CHUNKS + j, y_dev)
        zkeep[j] = ckeep[1, j, ours, :] + crecv[1, j, ours, :].astype(jnp.float32)
    for j in range(CHUNKS):
        total = zkeep[j]
        for k in range(3):
            arrive(brecv.at[k, j], sb, k * CHUNKS + j)
            total = total + brecv[k, j].astype(jnp.float32)
        zkeep[j] = total
        zsend[j] = total.astype(jnp.bfloat16)
        for d in range(nz - 1, 0, -1):
            src = zsend.at[j, pl.ds(pl.multiple_of(flip(d) * rows, rows), rows)]
            send(src, zrecv.at[j, d - 1], sz, j * nz + d, z_dev(d))
    for j in range(CHUNKS):
        total = zkeep[j, pl.ds(pl.multiple_of(z * rows, rows), rows), :]
        for d in range(1, nz):
            arrive(zrecv.at[j, d - 1], sz, j * nz + d)
            total = total + zrecv[j, d - 1].astype(jnp.float32)
        out[:, j * chunk : (j + 1) * chunk] = total.astype(jnp.bfloat16)
    for copy in sent:
        copy.wait_send()


def fused(tokens, norm_gain, token_expert_index, group_prob, expert_weight, w_gate, w_up, w_down):
    rows, width = tokens.shape
    n_ep, n_tp = lax.axis_size("ep"), lax.axis_size("tp")
    topk = token_expert_index.shape[1]
    ny = 2
    nz = n_ep // ny
    share, hidden = width // n_tp, w_gate.shape[2]
    chunk = share // CHUNKS
    all_rows = n_ep * rows
    half = nz * rows
    bf, f32 = jnp.bfloat16, jnp.float32
    vmem, dma = pltpu.VMEM, pltpu.SemaphoreType.DMA
    return pl.pallas_call(
        functools.partial(kernel, (nz, ny, rows, share, chunk)),
        out_shape=jax.ShapeDtypeStruct((rows, share), bf),
        in_specs=[pl.BlockSpec(memory_space=pltpu.HBM)] * 8,
        out_specs=pl.BlockSpec(memory_space=vmem),
        scratch_shapes=[
            vmem((rows, width), bf), vmem((1, width), f32), vmem((topk, rows), jnp.int32),
            vmem((1, rows), f32), vmem((topk, rows), f32),
            vmem((n_tp, all_rows, share), bf),
            vmem(w_gate.shape[1:], bf), vmem(w_up.shape[1:], bf), vmem(w_down.shape[1:], bf),
            vmem((n_ep, n_ep, LANES), f32),
            vmem((all_rows, hidden), f32), vmem((all_rows, hidden), f32), vmem((all_rows, hidden), bf),
            vmem((2, CHUNKS, all_rows, chunk), bf), vmem((2, CHUNKS, all_rows, chunk), bf),
            vmem((2, CHUNKS, all_rows, chunk), f32),
            vmem((CHUNKS, all_rows, chunk), bf), vmem((CHUNKS, half, chunk), bf), vmem((3, CHUNKS, half, chunk), bf),
            vmem((CHUNKS, half, chunk), bf), vmem((CHUNKS, nz - 1, rows, chunk), bf),
            vmem((CHUNKS, half, chunk), f32),
            dma((8,)), dma((2, nz)), dma((2, nz + 1)), dma((2, nz)), dma((2, nz)), dma((2, 2 * nz)), dma((2, 2 * nz)),
            dma((2, nz)), dma((2, nz)),
            dma((2, 2 * CHUNKS)), dma((2, 3 * CHUNKS)), dma((2, CHUNKS * nz)),
        ],
        compiler_params=pltpu.CompilerParams(
            collective_id=0, has_side_effects=True, vmem_limit_bytes=67043328
        ),
    )(tokens, norm_gain[None, :], token_expert_index.T, group_prob[None, :], expert_weight.T, w_gate, w_up, w_down)


def slots(rows, topk, experts):
    return min(rows, max(2, rows * topk // max(experts // GROUPS - topk, 1) + 1))


def body(*args):
    tokens, topk = args[0], args[2].shape[1]
    n_ep, n_tp = lax.axis_size("ep"), lax.axis_size("tp")
    rows, width = tokens.shape
    dense = slots(rows, topk, n_ep) == rows and n_ep > 1 and n_ep & (n_ep - 1) == 0 and n_tp == 4
    if dense and rows % 16 == 0 and width % (n_tp * CHUNKS * LANES) == 0:
        return fused(*args)
    return general(*args)


def solution(mesh):
    return jax.shard_map(
        body,
        mesh=mesh,
        in_specs=(
            P("ep", None),
            P(),
            P("ep", None),
            P("ep"),
            P("ep", None),
            P("ep", None, "tp"),
            P("ep", None, "tp"),
            P("ep", "tp", None),
        ),
        out_specs=P("ep", "tp"),
        check_vma=False,
    )
```

```python
import functools

import jax
import jax.numpy as jnp
from jax import lax
from jax.experimental import pallas as pl
from jax.experimental.pallas import tpu as pltpu
from jax.sharding import PartitionSpec as P

GROUPS = 2


def general(tokens, norm_gain, token_expert_index, group_prob, expert_weight, w_gate, w_up, w_down):
    rows_here, width = tokens.shape
    topk = token_expert_index.shape[1]
    experts = lax.axis_size("ep")
    tp_count = lax.axis_size("tp")
    per_group = experts // GROUPS
    capacity = min(rows_here, max(2, rows_here * topk // max(per_group - topk, 1) + 1))
    xf = tokens.astype(jnp.float32)
    normed = (xf * lax.rsqrt(jnp.mean(xf * xf, axis=-1, keepdims=True) + 1e-06) * norm_gain).astype(
        jnp.bfloat16
    )
    gates = group_prob[:, None] * expert_weight / jnp.sum(expert_weight, axis=-1, keepdims=True)
    flattened_index = token_expert_index.reshape(-1)
    onehot = (flattened_index[:, None] == jnp.arange(experts, dtype=jnp.int32)[None, :]).astype(
        jnp.int32
    )
    earlier = jnp.cumsum(onehot, axis=0) - onehot
    slot_rank = jnp.sum(earlier * onehot, axis=1)
    place = flattened_index * capacity + slot_rank
    slots_total = experts * capacity
    select = (jnp.arange(slots_total, dtype=jnp.int32)[:, None] == place[None, :]).astype(
        jnp.float32
    )
    select = jnp.sum(select.reshape(slots_total, rows_here, topk), axis=2).astype(jnp.bfloat16)
    outgoing = jnp.dot(select, normed, preferred_element_type=jnp.float32).astype(jnp.bfloat16)
    share = width // tp_count
    arrived = lax.all_to_all(outgoing, "ep", split_axis=0, concat_axis=0, tiled=True)
    gate = jnp.dot(arrived, w_gate[0], preferred_element_type=jnp.float32)
    upper = jnp.dot(arrived, w_up[0], preferred_element_type=jnp.float32)
    hidden = (jax.nn.silu(gate) * upper).astype(jnp.bfloat16)
    partial_out = jnp.dot(hidden, w_down[0], preferred_element_type=jnp.float32)
    mine = lax.psum_scatter(partial_out.astype(jnp.bfloat16), "tp", scatter_dimension=1, tiled=True)
    returned = lax.all_to_all(mine, "ep", split_axis=0, concat_axis=0, tiled=True)
    picked = returned[place].astype(jnp.float32).reshape(rows_here, topk, share)
    mixed = jnp.sum(picked * gates[:, :, None], axis=1)
    return mixed.astype(jnp.bfloat16)


MESH = pl.DeviceIdType.MESH
CHUNKS = 2
LANES = 128


def kernel(dims, tokens_hbm, gain_hbm, index_hbm, prob_hbm, weight_hbm, wg_hbm, wu_hbm, wd_hbm, out,
           tokens, gain, index, group_prob, weight, xg, wg, wu, wd, table, acc_g, acc_u, hid, csend, crecv, ckeep, bsend, ysend, brecv, zsend, zrecv, zkeep,
           wsem, gz, gy, gx, gw, gc, gd, tz, ty, sc, sb, sz):
    nz, ny, rows, share, chunk = dims
    ep, t = lax.axis_index("ep"), lax.axis_index("tp")
    z, y = ep // ny, ep % ny
    x, c = t // 2, t % 2
    yo = 1 - y
    t_core, t_x, t_diag = x * 2 + (1 - c), (1 - x) * 2 + c, (1 - x) * 2 + (1 - c)
    half = nz * rows
    y_dev = {"ep": z * ny + yo, "tp": t}
    x_dev = {"ep": ep, "tp": t_x}
    core_dev = {"ep": ep, "tp": t_core}

    diag_dev = {"ep": z * ny + yo, "tp": t_x}

    def flip(d):
        return sum(
            (1 << b) * (1 - (z // (1 << b)) % 2 if d >> b & 1 else (z // (1 << b)) % 2) for b in range(nz.bit_length() - 1)
        )

    def z_dev(d):
        return {"ep": flip(d) * ny + y, "tp": t}

    barrier = pltpu.get_barrier_semaphore()
    peers = [z_dev(d) for d in range(1, nz)] + [y_dev, x_dev, diag_dev, core_dev]
    for peer in peers:
        pl.semaphore_signal(barrier, inc=1, device_id=peer, device_id_type=MESH)

    loads = [
        pltpu.make_async_copy(wg_hbm.at[0], wg, wsem.at[0]),
        pltpu.make_async_copy(wu_hbm.at[0], wu, wsem.at[1]),
        pltpu.make_async_copy(wd_hbm.at[0], wd, wsem.at[2]),
    ]
    small = [
        pltpu.make_async_copy(src, dst, wsem.at[3 + i])
        for i, (src, dst) in enumerate(
            ((tokens_hbm, tokens), (gain_hbm, gain), (index_hbm, index), (prob_hbm, group_prob), (weight_hbm, weight))
        )
    ]
    for load in small + loads:
        load.start()

    def place(zz, yy):
        return pl.ds(pl.multiple_of((yy * nz + zz) * rows, rows), rows)

    for load in small:
        load.wait()
    xf = tokens[...].astype(jnp.float32)
    scale = lax.rsqrt(jnp.mean(xf * xf, axis=-1, keepdims=True) + 1e-06)
    normed = (xf * scale * gain[...]).astype(jnp.bfloat16)
    for q in range(xg.shape[0]):
        xg[q, place(z, y), :] = normed[:, q * share : (q + 1) * share]
    ew = weight[...]
    gates = group_prob[...] * ew / jnp.sum(ew, axis=0, keepdims=True)
    expert = lax.broadcasted_iota(jnp.int32, (table.shape[1], rows), 0)
    own = jnp.zeros(expert.shape, jnp.float32)
    for k in range(ew.shape[0]):
        own = own + jnp.where(index[k : k + 1, :] == expert, gates[k : k + 1, :], 0.0)
    table[y * nz + z] = jnp.zeros(table.shape[1:], jnp.float32)
    table[y * nz + z, :, :rows] = own
    pl.semaphore_wait(barrier, len(peers))

    sent = []

    def send(src, dst, sems, i, device):
        copy = pltpu.make_async_remote_copy(
            src_ref=src, dst_ref=dst, send_sem=sems.at[0, i], recv_sem=sems.at[1, i],
            device_id=device, device_id_type=MESH,
        )
        copy.start()
        sent.append(copy)

    def arrive(dst, sems, i):
        pltpu.make_async_remote_copy(
            src_ref=dst, dst_ref=dst, send_sem=sems.at[0, i], recv_sem=sems.at[1, i],
            device_id=y_dev, device_id_type=MESH,
        ).wait_recv()

    def block(q, zz, yy):
        return xg.at[q, place(zz, yy)]

    mine = block(t, z, y)
    for d in range(1, nz):
        send(mine, mine, gz, d, z_dev(d))
    send(mine, mine, gy, 0, y_dev)
    other = block(t_x, z, y)
    send(other, other, gy, nz, y_dev)
    my_table = table.at[y * nz + z]
    for d in range(1, nz):
        send(my_table, my_table, tz, d, z_dev(d))
    send(my_table, my_table, ty, 0, y_dev)

    def relay(got, sems, i, onward, k):
        arrive(got, sems, i)
        send(got, got, onward, k, core_dev)

    relay(block(t, z, yo), gy, 0, gc, nz)
    relay(block(t_x, z, yo), gy, nz, gd, nz)
    for d in range(1, nz):
        got = block(t, flip(d), y)
        arrive(got, gz, d)
        send(got, got, gw, d, diag_dev)
        send(got, got, gy, d, y_dev)
        send(got, got, gx, d, x_dev)
        send(got, got, gc, d, core_dev)
    for d in range(1, nz):
        got = table.at[y * nz + flip(d)]
        arrive(got, tz, d)
        send(got, got, ty, d, y_dev)

    def which(i):
        return (flip(i % nz), y if i < nz else yo)

    order = [nz] + list(range(1, nz)) + list(range(nz + 1, 2 * nz))

    def project(q, first):
        lhs = xg[q]
        span = pl.ds(pl.multiple_of(q * share, share), share)
        for acc, w in ((acc_g, wg), (acc_u, wu)):
            value = jnp.dot(lhs, w[span, :], preferred_element_type=jnp.float32)
            acc[...] = value if first else acc[...] + value

    loads[0].wait()
    loads[1].wait()
    for d in range(1, nz):
        relay(block(t_x, flip(d), y), gx, d, gd, d)
        relay(block(t, flip(d), yo), gy, d, gc, nz + d)
    project(t, True)
    for d in range(1, nz):
        relay(block(t_x, flip(d), yo), gw, d, gd, nz + d)
    for i in order:
        arrive(block(t_core, *which(i)), gc, i)
    project(t_core, False)
    project(t_x, False)
    for d in range(nz):
        arrive(table.at[yo * nz + flip(d)], ty, d)
    for i in order:
        arrive(block(t_diag, *which(i)), gd, i)
    project(t_diag, False)

    diagonal = lax.broadcasted_iota(jnp.int32, (rows, rows), 0) == lax.broadcasted_iota(jnp.int32, (rows, rows), 1)
    factor = jnp.concatenate(
        [
            jnp.sum(jnp.where(diagonal, table[b, pl.ds(ep, 1), :rows], 0.0), axis=1, keepdims=True)
            for b in range(table.shape[0])
        ],
        axis=0,
    )
    gate = acc_g[...]
    hid[...] = (gate / (1.0 + jnp.exp(-gate)) * acc_u[...] * factor).astype(jnp.bfloat16)

    loads[2].wait()

    def down(xq, cq, j):
        start = pl.multiple_of((xq * 2 + cq) * share + j * chunk, chunk)
        return jnp.dot(hid[...], wd[:, pl.ds(start, chunk)], preferred_element_type=jnp.float32)

    ours, theirs = pl.ds(pl.multiple_of(y * half, half), half), pl.ds(pl.multiple_of(yo * half, half), half)
    for j in range(CHUNKS):
        csend[0, j] = down(1 - x, 1 - c, j).astype(jnp.bfloat16)
        send(csend.at[0, j], crecv.at[0, j], sc, j, core_dev)
        csend[1, j] = down(x, 1 - c, j).astype(jnp.bfloat16)
        send(csend.at[1, j], crecv.at[1, j], sc, CHUNKS + j, core_dev)
    for j in range(CHUNKS):
        ckeep[0, j] = down(1 - x, c, j)
        ckeep[1, j] = down(x, c, j)
        arrive(crecv.at[0, j], sc, j)
        bsend[j] = (ckeep[0, j] + crecv[0, j].astype(jnp.float32)).astype(jnp.bfloat16)
        send(bsend.at[j, theirs], brecv.at[1, j], sb, CHUNKS + j, diag_dev)
        send(bsend.at[j, ours], brecv.at[0, j], sb, j, x_dev)
        arrive(crecv.at[1, j], sc, CHUNKS + j)
        ysend[j] = (ckeep[1, j, theirs, :] + crecv[1, j, theirs, :].astype(jnp.float32)).astype(jnp.bfloat16)
        send(ysend.at[j], brecv.at[2, j], sb, 2 * CHUNKS + j, y_dev)
        zkeep[j] = ckeep[1, j, ours, :] + crecv[1, j, ours, :].astype(jnp.float32)
    for j in range(CHUNKS):
        total = zkeep[j]
        for k in range(3):
            arrive(brecv.at[k, j], sb, k * CHUNKS + j)
            total = total + brecv[k, j].astype(jnp.float32)
        zkeep[j] = total
        zsend[j] = total.astype(jnp.bfloat16)
        for d in range(nz - 1, 0, -1):
            src = zsend.at[j, pl.ds(pl.multiple_of(flip(d) * rows, rows), rows)]
            send(src, zrecv.at[j, d - 1], sz, j * nz + d, z_dev(d))
    for j in range(CHUNKS):
        total = zkeep[j, pl.ds(pl.multiple_of(z * rows, rows), rows), :]
        for d in range(1, nz):
            arrive(zrecv.at[j, d - 1], sz, j * nz + d)
            total = total + zrecv[j, d - 1].astype(jnp.float32)
        out[:, j * chunk : (j + 1) * chunk] = total.astype(jnp.bfloat16)
    for copy in sent:
        copy.wait_send()


def fused(tokens, norm_gain, token_expert_index, group_prob, expert_weight, w_gate, w_up, w_down):
    rows, width = tokens.shape
    n_ep, n_tp = lax.axis_size("ep"), lax.axis_size("tp")
    topk = token_expert_index.shape[1]
    ny = 2
    nz = n_ep // ny
    share, hidden = width // n_tp, w_gate.shape[2]
    chunk = share // CHUNKS
    all_rows = n_ep * rows
    half = nz * rows
    bf, f32 = jnp.bfloat16, jnp.float32
    vmem, dma = pltpu.VMEM, pltpu.SemaphoreType.DMA
    return pl.pallas_call(
        functools.partial(kernel, (nz, ny, rows, share, chunk)),
        out_shape=jax.ShapeDtypeStruct((rows, share), bf),
        in_specs=[pl.BlockSpec(memory_space=pltpu.HBM)] * 8,
        out_specs=pl.BlockSpec(memory_space=vmem),
        scratch_shapes=[
            vmem((rows, width), bf), vmem((1, width), f32), vmem((topk, rows), jnp.int32),
            vmem((1, rows), f32), vmem((topk, rows), f32),
            vmem((n_tp, all_rows, share), bf),
            vmem(w_gate.shape[1:], bf), vmem(w_up.shape[1:], bf), vmem(w_down.shape[1:], bf),
            vmem((n_ep, n_ep, LANES), f32),
            vmem((all_rows, hidden), f32), vmem((all_rows, hidden), f32), vmem((all_rows, hidden), bf),
            vmem((2, CHUNKS, all_rows, chunk), bf), vmem((2, CHUNKS, all_rows, chunk), bf),
            vmem((2, CHUNKS, all_rows, chunk), f32),
            vmem((CHUNKS, all_rows, chunk), bf), vmem((CHUNKS, half, chunk), bf), vmem((3, CHUNKS, half, chunk), bf),
            vmem((CHUNKS, half, chunk), bf), vmem((CHUNKS, nz - 1, rows, chunk), bf),
            vmem((CHUNKS, half, chunk), f32),
            dma((8,)), dma((2, nz)), dma((2, nz + 1)), dma((2, nz)), dma((2, nz)), dma((2, 2 * nz)), dma((2, 2 * nz)),
            dma((2, nz)), dma((2, nz)),
            dma((2, 2 * CHUNKS)), dma((2, 3 * CHUNKS)), dma((2, CHUNKS * nz)),
        ],
        compiler_params=pltpu.CompilerParams(
            collective_id=0, has_side_effects=True, vmem_limit_bytes=67043328
        ),
    )(tokens, norm_gain[None, :], token_expert_index.T, group_prob[None, :], expert_weight.T, w_gate, w_up, w_down)


def slots(rows, topk, experts):
    return min(rows, max(2, rows * topk // max(experts // GROUPS - topk, 1) + 1))


def body(*args):
    tokens, topk = args[0], args[2].shape[1]
    n_ep, n_tp = lax.axis_size("ep"), lax.axis_size("tp")
    rows, width = tokens.shape
    dense = slots(rows, topk, n_ep) == rows and n_ep > 1 and n_ep & (n_ep - 1) == 0 and n_tp == 4
    if dense and rows % 16 == 0 and width % (n_tp * CHUNKS * LANES) == 0:
        return fused(*args)
    return general(*args)


def solution(mesh):
    return jax.shard_map(
        body,
        mesh=mesh,
        in_specs=(
            P("ep", None),
            P(),
            P("ep", None),
            P("ep"),
            P("ep", None),
            P("ep", None, "tp"),
            P("ep", None, "tp"),
            P("ep", "tp", None),
        ),
        out_specs=P("ep", "tp"),
        check_vma=False,
    )
```
